32 devices in a mesh: grp: 2 (over y), dp: 2 (over x), kv: 4 (over z), tp: 2 (over core).
Axes of the slice: x: 2, y: 2, z: 4, core: 2. Of those that a mesh axis runs over, the one named last changes fastest.
Arguments:
- tokens: bfloat16 [128, 2048], P(('grp', 'dp'), ('kv', 'tp')), parts along dimension 0, may hold values from -6 to 6
- norm_gain: float32 [2048], P('kv'), may hold values from 0.1 to 1.9
- w_query: bfloat16 [2048, 512], P('kv', 'tp'), may hold values from -0.125 to 0.125
- w_key: bfloat16 [2048, 512], P('kv', 'tp'), may hold values from -0.125 to 0.125
- w_value: bfloat16 [2048, 1024], P('kv', 'tp'), may hold values from -0.125 to 0.125
- w_outgate: bfloat16 [2048, 1024], P('kv', 'tp'), may hold values from -0.125 to 0.125
- w_ingate: bfloat16 [2048, 8], P('kv'), may hold values from -0.125 to 0.125
- w_forget: bfloat16 [2048, 8], P('kv'), may hold values from -0.125 to 0.125
- in_bias: float32 [8], replicated, may hold values from -1.5 to 0.5
- forget_bias: float32 [8], replicated, may hold values from -1 to 4
- memory: float32 [128, 8, 64, 128], P(('grp', 'dp', 'kv'), 'tp'), parts along dimension 0, may hold values from -4 to 4
- normalizer: float32 [128, 512], P(('grp', 'dp', 'kv'), 'tp'), parts along dimension 0, may hold values from -4 to 4
- stabilizer: float32 [128, 8], P(('grp', 'dp', 'kv'), 'tp'), parts along dimension 0, may hold values from -1 to 1
- w_out: bfloat16 [1024, 2048], P('tp', 'kv'), may hold values from -0.1875 to 0.1875
- mlp_gain: float32 [2048], replicated, may hold values from 0.1 to 1.9
- w_up: bfloat16 [2048, 8192], P(None, ('kv', 'tp')), may hold values from -0.125 to 0.125
- w_down: bfloat16 [8192, 2048], P(('kv', 'tp')), may hold values from -0.09375 to 0.09375
Outputs:
- mixed_out: bfloat16 [128, 2048], P(('grp', 'dp'), ('kv', 'tp')), parts along dimension 0
- memory_new: float32 [128, 8, 64, 128], P(('grp', 'dp', 'kv'), 'tp'), parts along dimension 0
- normalizer_new: float32 [128, 512], P(('grp', 'dp', 'kv'), 'tp'), parts along dimension 0
- stabilizer_new: float32 [128, 8], P(('grp', 'dp', 'kv'), 'tp'), parts along dimension 0
The draws below stay inside these ranges and needn't reach their ends.
There are 2 independent parts, one for each index of `grp`. The reference program is written for one: setup_inputs(seed, part) draws one part's arguments, and reference() takes and returns one part's arrays. A program takes and returns all parts, laid end to end along the dimension named above; an argument that names none is the same for every part. Nothing has to cross between parts.
All inputs are finite; a program needn't handle non-finite values.
Results may differ from the reference program's by a relative error of at most 0.03.
Values may be sent and summed in bfloat16 or wider, within the bound.
No kernel may reach another device: no remote copies, remote signals or barrier semaphores. Data moves between devices by JAX's collectives and lax.ppermute only.
A program may use at most 64 MiB of HBM per device.

```python
import jax
import jax.numpy as jnp
from jax import lax

D = 2048
HEADS = 8
QK_DIM = 64
VD_DIM = 128
FF = 8192
BATCH = 64
N_KV = 4
N_TP = 2


def with_spikes(drawn, stream_key, source, target, blocks, factor):
    owner, partner = [(jnp.arange(drawn.shape[dim]) // (drawn.shape[dim] // blocks)).reshape([-1 if axis == dim else 1 for axis in range(drawn.ndim)]) for dim in (source, target)]
    chosen = jax.random.permutation(stream_key, blocks)[partner]
    strong = (owner == chosen) | (owner == (partner + blocks // 2) % blocks)
    return jnp.where(strong, factor * drawn, drawn)


def block_levels(key, dims, cuts, smallest, largest):
    def one(dim, shards_of):
        heights = jax.random.uniform(jax.random.fold_in(jax.random.fold_in(key, 6), dim), (shards_of,), jnp.float32, smallest / len(cuts), largest / len(cuts))
        return jnp.repeat(jnp.exp(heights), dims[dim] // shards_of).reshape((-1,) + (1,) * (len(dims) - dim - 1))

    loudness = one(*cuts[0])
    for cut in cuts[1:]:
        loudness = loudness * one(*cut)
    return loudness


def bell_draw(own_key, shape, scale, most, split=(), held_as=jnp.bfloat16):
    gain = block_levels(own_key, shape, split, -0.22, 0.18) if split else 1.0
    result = jax.random.normal(own_key, shape, jnp.float32) * scale * gain
    return jnp.minimum(jnp.maximum(result, -most), most).astype(held_as)


def noise_with(key, dims, scale, most, cuts, heavy, dtype=jnp.bfloat16):
    values = scale * jax.random.normal(key, dims, jnp.float32)
    if cuts:
        values = values * block_levels(key, dims, cuts, -0.22, 0.18)
    return jnp.clip(with_spikes(values, jax.random.fold_in(key, 3), *heavy), -most, most).astype(dtype)


def setup_inputs(seed: int = 0, part: int = 0) -> dict:
    key_of = jax.random.split(jax.random.key(seed), 18)
    part_splits = jax.random.split(jax.random.fold_in(key_of[17], part), 18)
    tokens = noise_with(part_splits[0], (BATCH, D), 1.0, 6.0, ((0, 2), (1, 8)), (1, 0, 8, 2.0))
    norm_gain = jnp.clip(1.0 + 0.18 * jax.random.normal(key_of[1], (D,), jnp.float32), 0.1, 1.9)
    w_query = bell_draw(key_of[2], (D, HEADS * QK_DIM), D ** -0.5, 0.125, ((0, 4), (1, 2)))
    w_key = bell_draw(key_of[3], (D, HEADS * QK_DIM), D ** -0.5, 0.125, ((0, 4), (1, 2)))
    w_value = bell_draw(key_of[4], (D, HEADS * VD_DIM), D ** -0.5, 0.125, ((0, 4), (1, 2)))
    w_outgate = bell_draw(key_of[5], (D, HEADS * VD_DIM), D ** -0.5, 0.125, ((0, 4), (1, 2)))
    w_ingate = bell_draw(key_of[6], (D, HEADS), D ** -0.5, 0.125, ((0, 4),))
    w_forget = bell_draw(key_of[7], (D, HEADS), D ** -0.5, 0.125, ((0, 4),))
    in_bias = jnp.clip(jax.random.uniform(key_of[8], (HEADS,), jnp.float32, -1.5, 0.5), -1.5, 0.5)
    forget_bias = jnp.clip(jax.random.uniform(key_of[9], (HEADS,), jnp.float32, -1.0, 4.0), -1.0, 4.0)
    memory = bell_draw(part_splits[10], (BATCH, HEADS, QK_DIM, VD_DIM), 0.5, 4.0, ((0, 8), (1, 2)), jnp.float32)
    normalizer = bell_draw(part_splits[11], (BATCH, HEADS * QK_DIM), 0.5, 4.0, ((0, 8), (1, 2)), jnp.float32)
    stabilizer = jnp.clip(jax.random.uniform(part_splits[12], (BATCH, HEADS), jnp.float32, -1.0, 1.0) * block_levels(part_splits[12], (BATCH, HEADS), ((0, 8), (1, 2)), -0.4, 0.0), -1.0, 1.0)
    w_out = bell_draw(key_of[13], (HEADS * VD_DIM, D), (HEADS * VD_DIM) ** -0.5, 0.1875, ((0, 2), (1, 4)))
    mlp_gain = jnp.clip(1.0 + 0.18 * jax.random.normal(key_of[14], (D,), jnp.float32), 0.1, 1.9)
    w_up = bell_draw(key_of[15], (D, FF), D ** -0.5, 0.125, ((1, 8),))
    w_down = noise_with(key_of[16], (FF, D), FF ** -0.5, 0.09375, ((0, 8),), (0, 1, 8, 2.0))
    return dict(tokens=tokens, norm_gain=norm_gain, w_query=w_query, w_key=w_key, w_value=w_value, w_outgate=w_outgate, w_ingate=w_ingate, w_forget=w_forget, in_bias=in_bias, forget_bias=forget_bias, memory=memory, normalizer=normalizer, stabilizer=stabilizer, w_out=w_out, mlp_gain=mlp_gain, w_up=w_up, w_down=w_down)


EPSILON = 1e-06

def block_sum(left, weight, parts):
    rows = left.shape[0]
    width = weight.shape[0] // parts
    left_blocks = jnp.transpose(left.reshape(rows, parts, width), (1, 0, 2))
    weight_blocks = weight.reshape(parts, width, weight.shape[1])

    def step(total, pair):
        term = jnp.dot(pair[0], pair[1], preferred_element_type=jnp.float32).astype(jnp.bfloat16)
        term = lax.optimization_barrier(term)
        return (total + term.astype(jnp.float32), None)
    start = jnp.zeros((rows, weight.shape[1]), jnp.float32)
    total, unused = lax.scan(step, start, (left_blocks, weight_blocks))
    return total

def reference(tokens, norm_gain, w_query, w_key, w_value, w_outgate, w_ingate, w_forget, in_bias, forget_bias, memory, normalizer, stabilizer, w_out, mlp_gain, w_up, w_down):
    batch_rows = tokens.shape[0]
    tokens_f = tokens.astype(jnp.float32)
    rscale = lax.rsqrt(lax.optimization_barrier(jnp.mean(tokens_f * tokens_f, axis=1, keepdims=True)) + EPSILON)
    scaled = (tokens_f * norm_gain).astype(jnp.bfloat16)

    def product(weight):
        return block_sum(scaled, weight, N_KV) * rscale
    queries = product(w_query).reshape(batch_rows, HEADS, QK_DIM)
    keys_in = (product(w_key) * QK_DIM ** (-0.5)).reshape(batch_rows, HEADS, QK_DIM)
    values_in = product(w_value).reshape(batch_rows, HEADS, VD_DIM)
    out_pre = product(w_outgate).reshape(batch_rows, HEADS, VD_DIM)
    log_in = product(w_ingate) + in_bias
    log_forget = jax.nn.log_sigmoid(product(w_forget) + forget_bias)
    carried = log_forget + stabilizer
    stab_new = jnp.maximum(carried, log_in)
    take_new = jnp.exp(log_in - stab_new)
    keep_old = jnp.exp(carried - stab_new)
    norm_old = normalizer.reshape(batch_rows, HEADS, QK_DIM)
    score = lax.optimization_barrier(jnp.sum(queries * keys_in, axis=2))
    readout = jnp.einsum('shkv,shk->shv', memory, queries, precision=lax.Precision.HIGHEST)
    numer = (take_new * score)[..., None] * values_in + keep_old[..., None] * readout
    denom = take_new * score + keep_old * lax.optimization_barrier(jnp.sum(norm_old * queries, axis=2))
    cell = numer / jnp.maximum(jnp.abs(denom), 1.0)[..., None]
    hidden = (jax.nn.sigmoid(out_pre) * cell).reshape(batch_rows, HEADS * VD_DIM).astype(jnp.bfloat16)
    middle = (tokens_f + jnp.dot(hidden, w_out, preferred_element_type=jnp.float32)).astype(jnp.bfloat16)
    middle_f = middle.astype(jnp.float32)
    rscale_mid = lax.rsqrt(lax.optimization_barrier(jnp.mean(middle_f * middle_f, axis=1, keepdims=True)) + EPSILON)
    normed = (middle_f * rscale_mid * mlp_gain).astype(jnp.bfloat16)
    upward = jnp.dot(normed, w_up, preferred_element_type=jnp.float32)
    squared = jnp.square(jax.nn.relu(upward)).astype(jnp.bfloat16)
    mixed_out = (middle_f + block_sum(squared, w_down, N_KV * N_TP)).astype(jnp.bfloat16)
    memory_new = keep_old[..., None, None] * memory + take_new[..., None, None] * keys_in[..., :, None] * values_in[..., None, :]
    normalizer_new = (keep_old[..., None] * norm_old + take_new[..., None] * keys_in).reshape(batch_rows, HEADS * QK_DIM)
    return (mixed_out, memory_new, normalizer_new, stab_new)
```

```python
import itertools
import math

import jax
import jax.numpy as jnp
from jax import lax
from jax.sharding import PartitionSpec as P

EPSILON = 1e-06


def shifts(axes):
    sizes = [lax.axis_size(axis) for axis in axes]
    total = math.prod(sizes)

    def coords(linear):
        out = []
        for size in reversed(sizes):
            out.append(linear % size)
            linear //= size
        return out[::-1]

    def linear(where):
        out = 0
        for value, size in zip(where, sizes):
            out = out * size + value % size
        return out

    for step in range(1, total):
        offset = coords(step)
        perm = [
            (source, linear([a + b for a, b in zip(coords(source), offset)]))
            for source in range(total)
        ]
        own = [lax.axis_index(axis) for axis in axes]
        target = linear([a + b for a, b in zip(own, offset)])
        source = linear([a - b for a, b in zip(own, offset)])
        yield perm, target, source


def own_index(axes):
    out = 0
    for axis in axes:
        out = out * lax.axis_size(axis) + lax.axis_index(axis)
    return out


def scatter_pieces(array, axes, dim):
    count = math.prod(lax.axis_size(axis) for axis in axes)
    width = array.shape[dim] // count

    def piece(index):
        return lax.dynamic_slice_in_dim(array, index * width, width, dim)

    pieces = [
        lax.ppermute(piece(target), axes, perm) for perm, target, source in shifts(axes)
    ]
    return [piece(own_index(axes))] + pieces


def gather(array, axes, dim):
    count = math.prod(lax.axis_size(axis) for axis in axes)
    width = array.shape[dim]
    shape = list(array.shape)
    shape[dim] = width * count
    out = jnp.zeros(shape, array.dtype)
    out = lax.dynamic_update_slice_in_dim(out, array, own_index(axes) * width, dim)
    for perm, target, source in shifts(axes):
        out = lax.dynamic_update_slice_in_dim(
            out, lax.ppermute(array, axes, perm), source * width, dim
        )
    return out


def total_of(pieces):
    return sum(piece.astype(jnp.float32) for piece in pieces)


def channel_mix(rows_in, mlp_gain, w_up, w_down):
    rows_f = rows_in.astype(jnp.float32)
    rscale_mid = lax.rsqrt(jnp.mean(rows_f * rows_f, axis=1, keepdims=True) + EPSILON)
    normed = (rows_f * rscale_mid * mlp_gain).astype(jnp.bfloat16)
    upward = jnp.dot(normed, w_up, preferred_element_type=jnp.float32)
    squared = jnp.square(jax.nn.relu(upward)).astype(jnp.bfloat16)
    return jnp.dot(squared, w_down, preferred_element_type=jnp.float32).astype(jnp.bfloat16)


def hidden_blocks(hidden):
    kv_size = lax.axis_size("kv")
    tp_size = lax.axis_size("tp")
    rows = hidden.shape[0]
    axes = ("kv", "tp")
    blocks = []
    for tp_step in range(tp_size):
        out = jnp.zeros((rows * kv_size, hidden.shape[1]), hidden.dtype)
        for kv_step in range(kv_size):
            perm = [
                (
                    k * tp_size + t,
                    ((k + kv_step) % kv_size) * tp_size + (t + tp_step) % tp_size,
                )
                for k in range(kv_size)
                for t in range(tp_size)
            ]
            moved = lax.ppermute(hidden, axes, perm) if kv_step or tp_step else hidden
            source = (lax.axis_index("kv") - kv_step) % kv_size
            out = lax.dynamic_update_slice_in_dim(out, moved, source * rows, 0)
        blocks.append(out)
    return blocks


def shards(
    tokens,
    norm_gain,
    w_query,
    w_key,
    w_value,
    w_outgate,
    w_ingate,
    w_forget,
    in_bias,
    forget_bias,
    memory,
    normalizer,
    stabilizer,
    w_out,
    mlp_gain,
    w_up,
    w_down,
):
    local_heads = memory.shape[1]
    qk_width = memory.shape[2]
    model_width = mlp_gain.shape[0]
    own_columns = scatter_pieces(w_out, ("tp",), 1)
    own_rows = gather(tokens, ("tp",), 1)
    own_f = own_rows.astype(jnp.float32)
    scaled = (own_f * norm_gain).astype(jnp.bfloat16)

    def product(weight):
        return jnp.dot(scaled, weight, preferred_element_type=jnp.float32).astype(jnp.bfloat16)

    part_query = product(w_query)
    part_key = product(w_key)
    part_value = product(w_value)
    part_gate = product(w_outgate)
    part_input = product(w_ingate)
    part_forget = product(w_forget)
    part_squares = jnp.sum(own_f * own_f, axis=1, keepdims=True)
    upper_piece = part_squares.astype(jnp.bfloat16)
    rest_one = part_squares - upper_piece.astype(jnp.float32)
    middle_piece = rest_one.astype(jnp.bfloat16)
    lower_piece = (rest_one - middle_piece.astype(jnp.float32)).astype(jnp.bfloat16)
    pieces = jnp.concatenate([upper_piece, middle_piece, lower_piece], axis=1)
    parts = [part_query, part_key, part_value, part_gate, part_input, part_forget, pieces]
    packed = total_of(scatter_pieces(jnp.concatenate(parts, axis=1), ("kv",), 0))
    ends = list(itertools.accumulate(part.shape[1] for part in parts))
    sum_query, sum_key, sum_value, sum_gate, sum_input, sum_forget, square_parts = [
        packed[:, end - part.shape[1] : end] for part, end in zip(parts, ends)
    ]
    squares = jnp.sum(square_parts, axis=1)
    seq_rows = sum_query.shape[0]
    rscale = lax.rsqrt(squares / model_width + EPSILON)[:, None]
    queries = (sum_query * rscale).reshape(seq_rows, local_heads, qk_width)
    keys_in = (sum_key * rscale * qk_width ** (-0.5)).reshape(seq_rows, local_heads, qk_width)
    values_in = (sum_value * rscale).reshape(seq_rows, local_heads, -1)
    out_pre = (sum_gate * rscale).reshape(seq_rows, local_heads, -1)
    head_first = lax.axis_index("tp") * local_heads
    log_in = lax.dynamic_slice_in_dim(
        sum_input * rscale, head_first, local_heads, 1
    ) + lax.dynamic_slice_in_dim(in_bias, head_first, local_heads, 0)
    forget_arg = lax.dynamic_slice_in_dim(
        sum_forget * rscale, head_first, local_heads, 1
    ) + lax.dynamic_slice_in_dim(forget_bias, head_first, local_heads, 0)
    log_forget = jax.nn.log_sigmoid(forget_arg)
    carried = log_forget + stabilizer
    stab_new = jnp.maximum(carried, log_in)
    take_new = jnp.exp(log_in - stab_new)
    keep_old = jnp.exp(carried - stab_new)
    norm_old = normalizer.reshape(seq_rows, local_heads, qk_width)
    score = jnp.sum(queries * keys_in, axis=2)
    readout = jnp.einsum("shkv,shk->shv", memory, queries, precision=lax.Precision.HIGHEST)
    numer = (take_new * score)[..., None] * values_in + keep_old[..., None] * readout
    denom = take_new * score + keep_old * jnp.sum(norm_old * queries, axis=2)
    cell = numer / jnp.maximum(jnp.abs(denom), 1.0)[..., None]
    hidden = (jax.nn.sigmoid(out_pre) * cell).reshape(seq_rows, -1).astype(jnp.bfloat16)
    memory_new = (
        keep_old[..., None, None] * memory
        + take_new[..., None, None] * keys_in[..., :, None] * values_in[..., None, :]
    )
    normalizer_new = (keep_old[..., None] * norm_old + take_new[..., None] * keys_in).reshape(
        seq_rows, -1
    )
    whole_hidden = hidden_blocks(hidden)
    head_total = sum(
        jnp.dot(left, right, preferred_element_type=jnp.float32)
        for left, right in zip(whole_hidden, own_columns)
    )
    middle = (tokens.astype(jnp.float32) + head_total).astype(jnp.bfloat16)
    whole_mid = gather(middle, ("kv", "tp"), 1)
    branch = total_of(
        scatter_pieces(channel_mix(whole_mid, mlp_gain, w_up, w_down), ("kv", "tp"), 1)
    )
    mixed_out = (middle.astype(jnp.float32) + branch).astype(jnp.bfloat16)
    return (mixed_out, memory_new, normalizer_new, stab_new)


def solution(mesh):
    placed = (
        P(("grp", "dp"), ("kv", "tp")),
        P("kv"),
        P("kv", "tp"),
        P("kv", "tp"),
        P("kv", "tp"),
        P("kv", "tp"),
        P("kv", None),
        P("kv", None),
        P(),
        P(),
        P(("grp", "dp", "kv"), "tp", None, None),
        P(("grp", "dp", "kv"), "tp"),
        P(("grp", "dp", "kv"), "tp"),
        P("tp", "kv"),
        P(),
        P(None, ("kv", "tp")),
        P(("kv", "tp"), None),
    )
    return jax.shard_map(
        shards,
        mesh=mesh,
        in_specs=placed,
        out_specs=(
            P(("grp", "dp"), ("kv", "tp")),
            P(("grp", "dp", "kv"), "tp", None, None),
            P(("grp", "dp", "kv"), "tp"),
            P(("grp", "dp", "kv"), "tp"),
        ),
        check_vma=False,
    )
```

```python
import jax
import jax.numpy as jnp
from jax import lax
from jax.experimental import pallas as pl
from jax.experimental.pallas import tpu as pltpu
from jax.sharding import PartitionSpec as P

EPSILON = 1e-06


PAIRED = True


def steps_of(axis):
    size = lax.axis_size(axis)
    own = lax.axis_index(axis)
    paired = PAIRED and size & (size - 1) == 0
    for step in range(1, size):
        if paired:
            yield [(i, i ^ step) for i in range(size)], own ^ step, own ^ step
        else:
            perm = [(i, (i + step) % size) for i in range(size)]
            yield perm, (own + step) % size, (own - step) % size


def scatter_pieces(array, axis, dim):
    width = array.shape[dim] // lax.axis_size(axis)

    def piece(index):
        return lax.dynamic_slice_in_dim(array, index * width, width, dim)

    pieces = [
        lax.ppermute(piece(target), axis, perm) for perm, target, source in steps_of(axis)
    ]
    return [piece(lax.axis_index(axis))] + pieces


def gather_pieces(array, axis):
    return [array] + [lax.ppermute(array, axis, perm) for perm, target, source in steps_of(axis)]


def gather(array, axis, dim):
    width = array.shape[dim]
    shape = list(array.shape)
    shape[dim] = width * lax.axis_size(axis)
    own = lax.axis_index(axis)
    pieces = gather_pieces(array, axis)
    sources = [own] + [source for perm, target, source in steps_of(axis)]
    out = jnp.zeros(shape, array.dtype)
    for piece, source in zip(pieces, sources):
        out = lax.dynamic_update_slice_in_dim(out, piece, source * width, dim)
    return out


def total_of(pieces):
    return sum(piece.astype(jnp.float32) for piece in pieces)


def channel_mix(rows_in, mlp_gain, w_up, w_down):
    rows_f = rows_in.astype(jnp.float32)
    rscale_mid = lax.rsqrt(jnp.mean(rows_f * rows_f, axis=1, keepdims=True) + EPSILON)
    normed = (rows_f * rscale_mid * mlp_gain).astype(jnp.bfloat16)
    upward = jnp.dot(normed, w_up, preferred_element_type=jnp.float32)
    squared = jnp.square(jax.nn.relu(upward)).astype(jnp.bfloat16)
    return jnp.dot(squared, w_down, preferred_element_type=jnp.float32).astype(jnp.bfloat16)


LANES = 128


def in_vmem():
    return pl.BlockSpec(memory_space=pltpu.VMEM)


def in_smem():
    return pl.BlockSpec(memory_space=pltpu.SMEM)


def chosen(index, options):
    out = options[0]
    for number in range(1, len(options)):
        out = jnp.where(index == number, options[number], out)
    return out


def project(pieces, sources, norm_gain, weights):
    rows = pieces[0].shape[0]
    count = len(pieces)
    wide = [weight for weight in weights if weight.shape[1] % LANES == 0]
    narrow = [weight for weight in weights if weight.shape[1] % LANES]
    wide_end = sum(weight.shape[1] for weight in wide)
    narrow_end = sum(weight.shape[1] for weight in narrow) + 3
    padding = -narrow_end % LANES

    def body(*refs):
        source_ref, gain_ref, out_ref = refs[0], refs[1], refs[-1]
        piece_refs = refs[2 : 2 + count]
        weight_refs = refs[2 + count : -1]
        held = [ref[...].astype(jnp.float32) for ref in piece_refs]
        ordered = []
        for place in range(count):
            block = held[0]
            for number in range(1, count):
                block = jnp.where(source_ref[number] == place, held[number], block)
            ordered.append(block)
        own_f = jnp.concatenate(ordered, axis=1)
        scaled = (own_f * gain_ref[...]).astype(jnp.bfloat16)
        start = 0
        small = []
        for ref in weight_refs:
            part = jnp.dot(scaled, ref[...], preferred_element_type=jnp.float32)
            if ref.shape[1] % LANES == 0:
                out_ref[:, start : start + ref.shape[1]] = part.astype(jnp.bfloat16)
                start += ref.shape[1]
            else:
                small.append(part)
        squares = jnp.sum(own_f * own_f, axis=1, keepdims=True)
        upper = squares.astype(jnp.bfloat16).astype(jnp.float32)
        center = (squares - upper).astype(jnp.bfloat16).astype(jnp.float32)
        small += [upper, center, squares - upper - center]
        small.append(jnp.zeros((rows, padding), jnp.float32))
        out_ref[:, start:] = jnp.concatenate(small, axis=1).astype(jnp.bfloat16)

    return pl.pallas_call(
        body,
        out_shape=jax.ShapeDtypeStruct((rows, wide_end + narrow_end + padding), jnp.bfloat16),
        in_specs=[in_smem()] + [in_vmem()] * (1 + count + len(weights)),
        out_specs=in_vmem(),
        name="project",
    )(sources, norm_gain[None, :], *pieces, *wide, *narrow)


def cell_step(group, packed, in_bias, forget_bias, memory, normalizer, stabilizer, model_width):
    seqs, local_heads, qk_width, value_width = memory.shape
    heads = in_bias.shape[0]
    count = len(packed)
    qk_all = local_heads * qk_width
    value_all = local_heads * value_width

    def body(*refs):
        group_ref = refs[0]
        packed_refs = refs[1 : 1 + count]
        in_ref, forget_ref, memory_ref, norm_ref, stab_ref = refs[1 + count : 6 + count]
        hidden_ref, kept_ref, values_ref, keep_ref, norm_out_ref, stab_out_ref = refs[6 + count :]
        total = packed_refs[0][...].astype(jnp.float32)
        for ref in packed_refs[1:]:
            total = total + ref[...].astype(jnp.float32)
        gates = 2 * qk_all + 2 * value_all
        squares = jnp.sum(
            total[:, gates + 2 * heads : gates + 2 * heads + 3], axis=1, keepdims=True
        )
        rscale = lax.rsqrt(squares / model_width + EPSILON)
        queries = total[:, :qk_all] * rscale
        keys_in = total[:, qk_all : 2 * qk_all] * rscale * qk_width ** (-0.5)
        values_in = total[:, 2 * qk_all : 2 * qk_all + value_all] * rscale
        out_gate = jax.nn.sigmoid(total[:, 2 * qk_all + value_all : gates] * rscale)
        all_in = total[:, gates : gates + heads] * rscale + in_ref[...]
        all_forget = total[:, gates + heads : gates + 2 * heads] * rscale + forget_ref[...]

        def local(array):
            return chosen(
                group_ref[0],
                [array[:, at : at + local_heads] for at in range(0, heads, local_heads)],
            )

        log_in = local(all_in)
        forget_arg = local(all_forget)
        log_forget = jnp.minimum(forget_arg, 0.0) - jnp.log1p(jnp.exp(-jnp.abs(forget_arg)))
        carried = log_forget + stab_ref[...]
        stab_new = jnp.maximum(carried, log_in)
        take_new = jnp.exp(log_in - stab_new)
        keep_old = jnp.exp(carried - stab_new)
        stab_out_ref[...] = stab_new
        keep_ref[...] = keep_old
        values_ref[...] = values_in
        query_columns = jnp.transpose(queries)
        norm_old = norm_ref[...]
        for head in range(local_heads):
            span = slice(head * qk_width, (head + 1) * qk_width)
            lanes = slice(head * value_width, (head + 1) * value_width)
            take = take_new[:, head : head + 1]
            keep = keep_old[:, head : head + 1]
            taken = take * keys_in[:, span]
            kept_ref[:, span] = taken
            norm_out_ref[:, span] = keep * norm_old[:, span] + taken
            score = take * jnp.sum(queries[:, span] * keys_in[:, span], axis=1, keepdims=True)
            stored = keep * jnp.sum(norm_old[:, span] * queries[:, span], axis=1, keepdims=True)
            readout = jnp.concatenate(
                [
                    jnp.sum(
                        memory_ref[seq, head] * query_columns[span, seq : seq + 1],
                        axis=0,
                        keepdims=True,
                    )
                    for seq in range(seqs)
                ],
                axis=0,
            )
            numer = score * values_in[:, lanes] + keep * readout
            cell = numer / jnp.maximum(jnp.abs(score + stored), 1.0)
            hidden_ref[:, lanes] = (out_gate[:, lanes] * cell).astype(jnp.bfloat16)

    def shape(width, dtype=jnp.float32):
        return jax.ShapeDtypeStruct((seqs, width), dtype)

    return pl.pallas_call(
        body,
        out_shape=(
            shape(value_all, jnp.bfloat16),
            shape(qk_all),
            shape(value_all),
            shape(local_heads),
            shape(qk_all),
            shape(local_heads),
        ),
        in_specs=[in_smem()] + [in_vmem()] * (count + 5),
        out_specs=(in_vmem(),) * 6,
        name="cell_step",
    )(
        group,
        *packed,
        in_bias[None, :],
        forget_bias[None, :],
        memory,
        normalizer,
        stabilizer,
    )


def shards(
    tokens,
    norm_gain,
    w_query,
    w_key,
    w_value,
    w_outgate,
    w_ingate,
    w_forget,
    in_bias,
    forget_bias,
    memory,
    normalizer,
    stabilizer,
    w_out,
    mlp_gain,
    w_up,
    w_down,
):
    kv_size = lax.axis_size("kv")
    tp_size = lax.axis_size("tp")
    local_heads = memory.shape[1]
    qk_width = memory.shape[2]
    model_width = mlp_gain.shape[0]
    own_columns = scatter_pieces(w_out, "tp", 1)
    own_group = lax.axis_index("tp")
    sources = jnp.stack(
        [own_group] + [source for perm, target, source in steps_of("tp")]
    ).astype(jnp.int32)
    packed = project(
        gather_pieces(tokens, "tp"),
        sources,
        norm_gain,
        [w_query, w_key, w_value, w_outgate, w_ingate, w_forget],
    )
    hidden, taken, values_in, keep_old, normalizer_new, stab_new = cell_step(
        sources[:1],
        scatter_pieces(packed, "kv", 0),
        in_bias,
        forget_bias,
        memory,
        normalizer,
        stabilizer,
        model_width,
    )
    seq_rows = hidden.shape[0]
    memory_new = (
        keep_old[..., None, None] * memory
        + taken.reshape(seq_rows, local_heads, qk_width)[..., None]
        * values_in.reshape(seq_rows, local_heads, 1, -1)
    )
    head_total = sum(
        jnp.dot(left, right, preferred_element_type=jnp.float32)
        for left, right in zip(gather_pieces(gather(hidden, "kv", 0), "tp"), own_columns)
    )
    middle = (tokens.astype(jnp.float32) + head_total).astype(jnp.bfloat16)
    blocks = jnp.split(gather(gather(middle, "kv", 1), "tp", 1), kv_size * tp_size, axis=1)
    whole_mid = jnp.concatenate(
        [blocks[t * kv_size + k] for k in range(kv_size) for t in range(tp_size)], axis=1
    )
    partial = channel_mix(whole_mid, mlp_gain, w_up, w_down)
    rows = partial.shape[0]
    by_owner = partial.reshape(rows, kv_size, -1)
    chip_sum = total_of(scatter_pieces(by_owner, "tp", 2)).astype(jnp.bfloat16)
    branch = total_of(scatter_pieces(chip_sum, "kv", 1)).reshape(rows, -1)
    mixed_out = (middle.astype(jnp.float32) + branch).astype(jnp.bfloat16)
    return (mixed_out, memory_new, normalizer_new, stab_new)


def solution(mesh):
    placed = (
        P(("grp", "dp"), ("kv", "tp")),
        P("kv"),
        P("kv", "tp"),
        P("kv", "tp"),
        P("kv", "tp"),
        P("kv", "tp"),
        P("kv", None),
        P("kv", None),
        P(),
        P(),
        P(("grp", "dp", "kv"), "tp", None, None),
        P(("grp", "dp", "kv"), "tp"),
        P(("grp", "dp", "kv"), "tp"),
        P("tp", "kv"),
        P(),
        P(None, ("kv", "tp")),
        P(("kv", "tp"), None),
    )
    return jax.shard_map(
        shards,
        mesh=mesh,
        in_specs=placed,
        out_specs=(
            P(("grp", "dp"), ("kv", "tp")),
            P(("grp", "dp", "kv"), "tp", None, None),
            P(("grp", "dp", "kv"), "tp"),
            P(("grp", "dp", "kv"), "tp"),
        ),
        check_vma=False,
    )
```

```python
import jax
import jax.numpy as jnp
from jax import lax
from jax.experimental import pallas as pl
from jax.experimental.pallas import tpu as pltpu
from jax.sharding import PartitionSpec as P

EPSILON = 1e-06


PAIRED = True


def steps_of(axis):
    size = lax.axis_size(axis)
    own = lax.axis_index(axis)
    paired = PAIRED and size & (size - 1) == 0
    for step in range(1, size):
        if paired:
            yield [(i, i ^ step) for i in range(size)], own ^ step, own ^ step
        else:
            perm = [(i, (i + step) % size) for i in range(size)]
            yield perm, (own + step) % size, (own - step) % size


def scatter_pieces(array, axis, dim):
    width = array.shape[dim] // lax.axis_size(axis)

    def piece(index):
        return lax.dynamic_slice_in_dim(array, index * width, width, dim)

    pieces = [
        lax.ppermute(piece(target), axis, perm) for perm, target, source in steps_of(axis)
    ]
    return [piece(lax.axis_index(axis))] + pieces


def gather_pieces(array, axis):
    return [array] + [lax.ppermute(array, axis, perm) for perm, target, source in steps_of(axis)]


def gather(array, axis, dim):
    width = array.shape[dim]
    shape = list(array.shape)
    shape[dim] = width * lax.axis_size(axis)
    own = lax.axis_index(axis)
    pieces = gather_pieces(array, axis)
    sources = [own] + [source for perm, target, source in steps_of(axis)]
    out = jnp.zeros(shape, array.dtype)
    for piece, source in zip(pieces, sources):
        out = lax.dynamic_update_slice_in_dim(out, piece, source * width, dim)
    return out


def total_of(pieces):
    return sum(piece.astype(jnp.float32) for piece in pieces)


def channel_mix(rows_in, mlp_gain, w_up, w_down):
    rows_f = rows_in.astype(jnp.float32)
    rscale_mid = lax.rsqrt(jnp.mean(rows_f * rows_f, axis=1, keepdims=True) + EPSILON)
    normed = (rows_f * rscale_mid * mlp_gain).astype(jnp.bfloat16)
    upward = jnp.dot(normed, w_up, preferred_element_type=jnp.float32)
    squared = jnp.square(jax.nn.relu(upward)).astype(jnp.bfloat16)
    return jnp.dot(squared, w_down, preferred_element_type=jnp.float32).astype(jnp.bfloat16)


LANES = 128


def in_vmem():
    return pl.BlockSpec(memory_space=pltpu.VMEM)


def in_smem():
    return pl.BlockSpec(memory_space=pltpu.SMEM)


def chosen(index, options):
    out = options[0]
    for number in range(1, len(options)):
        out = jnp.where(index == number, options[number], out)
    return out


def project(pieces, sources, targets, norm_gain, weights):
    rows = pieces[0].shape[0]
    count = len(pieces)
    wide = [weight for weight in weights if weight.shape[1] % LANES == 0]
    narrow = [weight for weight in weights if weight.shape[1] % LANES]
    wide_end = sum(weight.shape[1] for weight in wide)
    narrow_end = sum(weight.shape[1] for weight in narrow) + 3
    padding = -narrow_end % LANES
    seqs = rows // targets.shape[0]
    width = wide_end + narrow_end + padding

    def body(*refs):
        source_ref, target_ref, gain_ref, all_ref = refs[0], refs[1], refs[2], refs[-1]
        piece_refs = refs[3 : 3 + count]
        weight_refs = refs[3 + count : 3 + count + len(weights)]
        out_refs = refs[3 + count + len(weights) : -1]
        held = [ref[...].astype(jnp.float32) for ref in piece_refs]
        ordered = []
        for place in range(count):
            block = held[0]
            for number in range(1, count):
                block = jnp.where(source_ref[number] == place, held[number], block)
            ordered.append(block)
        own_f = jnp.concatenate(ordered, axis=1)
        scaled = (own_f * gain_ref[...]).astype(jnp.bfloat16)
        start = 0
        small = []
        for ref in weight_refs:
            if ref.shape[0] == scaled.shape[1]:
                part = jnp.dot(scaled, ref[...], preferred_element_type=jnp.float32)
                all_ref[:, start : start + ref.shape[1]] = part
                start += ref.shape[1]
            else:
                small.append(
                    lax.dot_general(
                        scaled,
                        ref[...],
                        (((1,), (1,)), ((), ())),
                        preferred_element_type=jnp.float32,
                    )
                )
        squares = jnp.sum(own_f * own_f, axis=1, keepdims=True)
        upper = squares.astype(jnp.bfloat16).astype(jnp.float32)
        center = (squares - upper).astype(jnp.bfloat16).astype(jnp.float32)
        small += [upper, center, squares - upper - center]
        small.append(jnp.zeros((rows, padding), jnp.float32))
        all_ref[:, start:] = jnp.concatenate(small, axis=1)
        for number, ref in enumerate(out_refs):
            first = pl.multiple_of(target_ref[number] * seqs, seqs)
            ref[...] = all_ref[pl.ds(first, seqs), :].astype(jnp.bfloat16)

    return pl.pallas_call(
        body,
        out_shape=(jax.ShapeDtypeStruct((seqs, width), jnp.bfloat16),) * targets.shape[0],
        in_specs=[in_smem()] * 2 + [in_vmem()] * (1 + count + len(weights)),
        out_specs=(in_vmem(),) * targets.shape[0],
        scratch_shapes=[pltpu.VMEM((rows, width), jnp.float32)],
        name="project",
    )(sources, targets, norm_gain[None, :], *pieces, *wide, *[weight.T for weight in narrow])


def cell_step(group, packed, in_bias, forget_bias, memory, normalizer, stabilizer, model_width):
    seqs, local_heads, qk_width, value_width = memory.shape
    heads = in_bias.shape[0]
    count = len(packed)
    qk_all = local_heads * qk_width
    value_all = local_heads * value_width

    def body(*refs):
        group_ref = refs[0]
        packed_refs = refs[1 : 1 + count]
        in_ref, forget_ref, memory_ref, norm_ref, stab_ref = refs[1 + count : 6 + count]
        hidden_ref, kept_ref, values_ref, keep_ref, norm_out_ref, stab_out_ref = refs[6 + count :]
        total = packed_refs[0][...].astype(jnp.float32)
        for ref in packed_refs[1:]:
            total = total + ref[...].astype(jnp.float32)
        gates = 2 * qk_all + 2 * value_all
        squares = jnp.sum(
            total[:, gates + 2 * heads : gates + 2 * heads + 3], axis=1, keepdims=True
        )
        rscale = lax.rsqrt(squares / model_width + EPSILON)
        queries = total[:, :qk_all] * rscale
        keys_in = total[:, qk_all : 2 * qk_all] * rscale * qk_width ** (-0.5)
        values_in = total[:, 2 * qk_all : 2 * qk_all + value_all] * rscale
        out_gate = jax.nn.sigmoid(total[:, 2 * qk_all + value_all : gates] * rscale)
        all_in = total[:, gates : gates + heads] * rscale + in_ref[...]
        all_forget = total[:, gates + heads : gates + 2 * heads] * rscale + forget_ref[...]

        def local(array):
            return chosen(
                group_ref[0],
                [array[:, at : at + local_heads] for at in range(0, heads, local_heads)],
            )

        log_in = local(all_in)
        forget_arg = local(all_forget)
        log_forget = jnp.minimum(forget_arg, 0.0) - jnp.log1p(jnp.exp(-jnp.abs(forget_arg)))
        carried = log_forget + stab_ref[...]
        stab_new = jnp.maximum(carried, log_in)
        take_new = jnp.exp(log_in - stab_new)
        keep_old = jnp.exp(carried - stab_new)
        stab_out_ref[...] = stab_new
        keep_ref[...] = keep_old
        values_ref[...] = values_in
        query_columns = jnp.transpose(queries)
        norm_old = norm_ref[...]
        for head in range(local_heads):
            span = slice(head * qk_width, (head + 1) * qk_width)
            lanes = slice(head * value_width, (head + 1) * value_width)
            take = take_new[:, head : head + 1]
            keep = keep_old[:, head : head + 1]
            taken = take * keys_in[:, span]
            kept_ref[:, span] = taken
            norm_out_ref[:, span] = keep * norm_old[:, span] + taken
            score = take * jnp.sum(queries[:, span] * keys_in[:, span], axis=1, keepdims=True)
            stored = keep * jnp.sum(norm_old[:, span] * queries[:, span], axis=1, keepdims=True)
            readout = jnp.concatenate(
                [
                    jnp.sum(
                        memory_ref[seq, head] * query_columns[span, seq : seq + 1],
                        axis=0,
                        keepdims=True,
                    )
                    for seq in range(seqs)
                ],
                axis=0,
            )
            numer = score * values_in[:, lanes] + keep * readout
            cell = numer / jnp.maximum(jnp.abs(score + stored), 1.0)
            hidden_ref[:, lanes] = (out_gate[:, lanes] * cell).astype(jnp.bfloat16)

    def shape(width, dtype=jnp.float32):
        return jax.ShapeDtypeStruct((seqs, width), dtype)

    return pl.pallas_call(
        body,
        out_shape=(
            shape(value_all, jnp.bfloat16),
            shape(qk_all),
            shape(value_all),
            shape(local_heads),
            shape(qk_all),
            shape(local_heads),
        ),
        in_specs=[in_smem()] + [in_vmem()] * (count + 5),
        out_specs=(in_vmem(),) * 6,
        name="cell_step",
    )(
        group,
        *packed,
        in_bias[None, :],
        forget_bias[None, :],
        memory,
        normalizer,
        stabilizer,
    )


def shards(
    tokens,
    norm_gain,
    w_query,
    w_key,
    w_value,
    w_outgate,
    w_ingate,
    w_forget,
    in_bias,
    forget_bias,
    memory,
    normalizer,
    stabilizer,
    w_out,
    mlp_gain,
    w_up,
    w_down,
):
    kv_size = lax.axis_size("kv")
    tp_size = lax.axis_size("tp")
    local_heads = memory.shape[1]
    qk_width = memory.shape[2]
    model_width = mlp_gain.shape[0]
    own_columns = scatter_pieces(w_out, "tp", 1)
    own_group = lax.axis_index("tp")
    sources = jnp.stack(
        [own_group] + [source for perm, target, source in steps_of("tp")]
    ).astype(jnp.int32)
    targets = jnp.stack(
        [lax.axis_index("kv")] + [target for perm, target, source in steps_of("kv")]
    ).astype(jnp.int32)
    packed = project(
        gather_pieces(tokens, "tp"),
        sources,
        targets,
        norm_gain,
        [w_query, w_key, w_value, w_outgate, w_ingate, w_forget],
    )
    hidden, taken, values_in, keep_old, normalizer_new, stab_new = cell_step(
        sources[:1],
        packed[:1]
        + tuple(
            lax.ppermute(part, "kv", perm)
            for part, (perm, target, source) in zip(packed[1:], steps_of("kv"))
        ),
        in_bias,
        forget_bias,
        memory,
        normalizer,
        stabilizer,
        model_width,
    )
    seq_rows = hidden.shape[0]
    memory_new = (
        keep_old[..., None, None] * memory
        + taken.reshape(seq_rows, local_heads, qk_width)[..., None]
        * values_in.reshape(seq_rows, local_heads, 1, -1)
    )
    head_total = sum(
        jnp.dot(left, right, preferred_element_type=jnp.float32)
        for left, right in zip(gather_pieces(gather(hidden, "kv", 0), "tp"), own_columns)
    )
    middle = (tokens.astype(jnp.float32) + head_total).astype(jnp.bfloat16)
    blocks = jnp.split(gather(gather(middle, "kv", 1), "tp", 1), kv_size * tp_size, axis=1)
    whole_mid = jnp.concatenate(
        [blocks[t * kv_size + k] for k in range(kv_size) for t in range(tp_size)], axis=1
    )
    partial = channel_mix(whole_mid, mlp_gain, w_up, w_down)
    rows = partial.shape[0]
    by_owner = partial.reshape(rows, kv_size, -1)
    chip_sum = total_of(scatter_pieces(by_owner, "tp", 2)).astype(jnp.bfloat16)
    branch = total_of(scatter_pieces(chip_sum, "kv", 1)).reshape(rows, -1)
    mixed_out = (middle.astype(jnp.float32) + branch).astype(jnp.bfloat16)
    return (mixed_out, memory_new, normalizer_new, stab_new)


def solution(mesh):
    placed = (
        P(("grp", "dp"), ("kv", "tp")),
        P("kv"),
        P("kv", "tp"),
        P("kv", "tp"),
        P("kv", "tp"),
        P("kv", "tp"),
        P("kv", None),
        P("kv", None),
        P(),
        P(),
        P(("grp", "dp", "kv"), "tp", None, None),
        P(("grp", "dp", "kv"), "tp"),
        P(("grp", "dp", "kv"), "tp"),
        P("tp", "kv"),
        P(),
        P(None, ("kv", "tp")),
        P(("kv", "tp"), None),
    )
    return jax.shard_map(
        shards,
        mesh=mesh,
        in_specs=placed,
        out_specs=(
            P(("grp", "dp"), ("kv", "tp")),
            P(("grp", "dp", "kv"), "tp", None, None),
            P(("grp", "dp", "kv"), "tp"),
            P(("grp", "dp", "kv"), "tp"),
        ),
        check_vma=False,
    )
```
